128 devices in a mesh: sp: 16 (over z, x), dp: 8 (over y, core).
Axes of the slice: x: 4, y: 4, z: 4, core: 2. Of those that a mesh axis runs over, the one named last changes fastest.
Arguments:
- residual_in: bfloat16 [8, 2048, 2048], P('dp', 'sp'), may hold values from -6 to 6
- query_rows: bfloat16 [8, 2048, 1024], P('dp', 'sp'), may hold values from -40 to 40
- key_rows: bfloat16 [8, 2048, 1024], P('dp', 'sp'), may hold values from -40 to 40
- value_rows: bfloat16 [8, 2048, 1024], P('dp', 'sp'), may hold values from -6 to 6
- gate_sums: float32 [8, 16, 2048], P('dp', 'sp'), as said below
- out_weight: bfloat16 [1024, 2048], replicated, may hold values from -0.1875 to 0.1875
- mix_gain: float32 [2048], replicated, may hold values from 0.1 to 1.9
- ffn_gain: float32 [2048], replicated, may hold values from 0.1 to 1.9
- expert_ids: int32 [8, 2048, 4], P('dp', 'sp'), may hold values from 0 to 127, all different within a row; in each aligned block of 128 rows (0 to 127, 128 to 255, ..., all dimensions but the last counted through in order) at most 8 rows name the same one
- route_weights: float32 [8, 2048, 4], P('dp', 'sp'), may hold values from 0.3 to 2
- expert_gate: bfloat16 [128, 2048, 512], P(('sp', 'dp')), may hold values from -0.125 to 0.125
- expert_up: bfloat16 [128, 2048, 512], P(('sp', 'dp')), may hold values from -0.125 to 0.125
- expert_down: bfloat16 [128, 512, 2048], P(('sp', 'dp')), may hold values from -0.25 to 0.25
- shared_gate: bfloat16 [2048, 512], replicated, may hold values from -0.125 to 0.125
- shared_up: bfloat16 [2048, 512], replicated, may hold values from -0.125 to 0.125
- shared_down: bfloat16 [512, 2048], replicated, may hold values from -0.25 to 0.25
Outputs:
- result_rows: bfloat16 [8, 2048, 2048], P('dp', 'sp')
The draws below stay inside these ranges and needn't reach their ends.
Inputs may be any that keep to these rules, and one draw needn't show every extreme that they name: `expert_ids`: each row names 4 different experts. In the rows of one device no expert is named more than 8 times, a bound that some block reaches in some devices' rows. `gate_sums`: Non-increasing along positions for every sequence and head.
All inputs are finite; a program needn't handle non-finite values.
Results may differ from the reference program's by a relative error of at most 0.0071.
Values may be sent and summed in bfloat16 or wider, within the bound.
A program may use at most 128 MiB of HBM per device.

```python
import math
import jax
import jax.numpy as jnp
import numpy as np
from jax import lax

D = 2048
HEADS = 16
HEAD_DIM = 64
EFF = 512
TOPK = 4
TOK_DEV = 128
ATT = 1024
SEQUENCE_COUNT = 8
SEQUENCE_LENGTH = 2048
EXPERTS = 128
CAP = 8


def drawn(key):
    base = jax.random.fold_in(key, 17)
    first, second = jax.random.split(base, 2)
    query_draw = jnp.clip(jax.random.normal(first, (SEQUENCE_COUNT, SEQUENCE_LENGTH, ATT), jnp.float32), -6.0, 6.0)
    key_draw = jnp.clip(jax.random.normal(second, (SEQUENCE_COUNT, SEQUENCE_LENGTH, ATT), jnp.float32), -6.0, 6.0)
    return (query_draw, key_draw)


def draw_query_rows(key, part):
    return drawn(key)[0].astype(jnp.bfloat16)


def draw_key_rows(key, part):
    return drawn(key)[1].astype(jnp.bfloat16)


def draw_gate_sums(key, part):
    base = jax.random.fold_in(key, 29)
    first, second, third, fourth, fifth, sixth_draw, seventh_draw = jax.random.split(base, 7)
    order = jax.random.permutation(first, HEADS)
    fast = order < HEADS // 2
    fast_rate = jnp.exp(jax.random.uniform(second, (SEQUENCE_COUNT, HEADS), jnp.float32, jnp.log(1.0 / 60.0), jnp.log(1.0 / 25.0)))
    slow_total = jnp.exp(jax.random.uniform(third, (SEQUENCE_COUNT, HEADS), jnp.float32, jnp.log(0.2), jnp.log(0.8)))
    rate = jnp.where(fast[None, :], fast_rate, slow_total / SEQUENCE_LENGTH)
    rough = jnp.exp(jax.random.uniform(fourth, (SEQUENCE_COUNT, HEADS, SEQUENCE_LENGTH), jnp.float32, jnp.log(0.5), jnp.log(2.0)))
    block_factor = jnp.exp(jax.random.uniform(fifth, (SEQUENCE_COUNT, SEQUENCE_LENGTH // TOK_DEV), jnp.float32, 0.0, jnp.log(3.0)))
    block_factor = jnp.repeat(block_factor, TOK_DEV, axis=1)
    step_values = -rate[:, :, None] * rough * block_factor[:, None, :]
    spike_position = jax.random.randint(sixth_draw, (SEQUENCE_COUNT, 3), 0, SEQUENCE_LENGTH)
    spike_length = jnp.log(jax.random.uniform(seventh_draw, (SEQUENCE_COUNT, 3), jnp.float32, 0.5, 0.8))
    token_positions = jnp.arange(SEQUENCE_LENGTH)
    match_count = jnp.sum(jnp.where(token_positions[None, None, :] == spike_position[:, :, None], spike_length[:, :, None], 0.0), axis=1)
    slow_mask = jnp.where(fast, 0.0, 1.0)
    step_values = step_values + slow_mask[None, :, None] * match_count[:, None, :]
    return jnp.cumsum(step_values, axis=2)


def block_scale(rng, shape, cuts, smallest, largest):
    def one(position, parts):
        heights = jax.random.uniform(jax.random.fold_in(jax.random.fold_in(rng, 6), position), (parts,), jnp.float32, smallest / len(cuts), largest / len(cuts))
        return jnp.repeat(jnp.exp(heights), shape[position] // parts).reshape((-1,) + (1,) * (len(shape) - position - 1))

    level = one(*cuts[0])
    for cut in cuts[1:]:
        level = level * one(*cut)
    return level


def assign_block(rng, own, number, rows, number_of, top, reach, lean):
    ranking = jax.random.permutation(rng, number_of)
    packed, usual = load_shares(number_of, rows * top, reach, lean, True), load_shares(number_of, rows * top, reach, lean, False)
    places = jnp.arange(number_of)

    def named(tallies, rotation):
        used = int((tallies > 0).sum())
        fixed = max(1, used // 4)
        passed = fixed + (places - fixed + rotation * (used - fixed)) % max(1, number_of - fixed)
        return jnp.zeros((number_of,), jnp.int32).at[ranking[jnp.where(places < fixed, places, passed)]].set(jnp.asarray(tallies, jnp.int32))

    tallies = jnp.where(number % 4 == 0, named(packed, number // 4), named(usual, number - number // 4 - 1))
    mixed = jax.random.permutation(jax.random.fold_in(own, 3), number_of)
    source_of, receiver = mixed[0:number_of // 2 * 2:2], mixed[1:number_of // 2 * 2:2]
    slack = jnp.minimum(tallies[source_of] - 1, reach - tallies[receiver]) // 2
    slack = jnp.where((source_of == ranking[0]) | (receiver == ranking[0]) | (tallies[receiver] == 0), 0, jnp.maximum(slack, 0))
    passed = jax.random.randint(jax.random.fold_in(own, 4), (number_of // 2,), 0, 1 << 20) % (slack + 1)
    tallies = tallies.at[source_of].add(-passed).at[receiver].add(passed)
    labels = jnp.searchsorted(jnp.cumsum(tallies), jnp.arange(rows * top), side="right").astype(jnp.int32)
    listing = labels.reshape(top, rows).T
    listing = listing[jax.random.permutation(jax.random.fold_in(own, 1), rows)]
    rotation = jax.random.randint(jax.random.fold_in(own, 2), (rows, 1), 0, top)
    return jnp.take_along_axis(listing, (jnp.arange(top)[None, :] + rotation) % top, axis=1)


def load_shares(count, total, limit, skew, full):
    portions = [(1 << 20) // math.isqrt(standing ** skew) + 1 for standing in range(1, count + 1)]
    largest = limit if full else min(limit, max(-(-total // count), total * portions[0] // sum(portions)))
    least = 1 if total - largest >= count - 1 else 0
    given, spare = [largest] + [least] * (count - 1), total - largest - least * (count - 1)
    while spare > 0:
        movable = [i for i in range(1, count) if given[i] < largest] or [i for i in range(1, count) if given[i] < limit]
        mass, remaining = sum([portions[i] for i in movable]), spare
        for i in movable:
            addition = min(limit - given[i], max(1, remaining * portions[i] // mass), spare)
            given[i] = given[i] + addition
            spare = spare - addition
    return np.array(given)


def centred(key, shape, deviation, most, pieces=(), kind=jnp.bfloat16):
    result = deviation * jax.random.normal(key, shape, jnp.float32)
    if pieces:
        result = result * block_scale(key, shape, pieces, -0.22, 0.18)
    return jnp.clip(result, -most, most).astype(kind)


def setup_inputs(seed: int = 0) -> dict:
    keys = jax.random.split(jax.random.key(seed), 17)
    residual_in = centred(keys[0], (SEQUENCE_COUNT, SEQUENCE_LENGTH, D), 1.0, 6.0, ((0, 8), (1, 16)))
    query_rows = draw_query_rows(jax.random.fold_in(keys[16], 71), 0)
    key_rows = draw_key_rows(jax.random.fold_in(keys[16], 71), 0)
    value_rows = centred(keys[3], (SEQUENCE_COUNT, SEQUENCE_LENGTH, ATT), 1.0, 6.0, ((0, 8), (1, 16)))
    gate_sums = draw_gate_sums(jax.random.fold_in(keys[16], 71), 0)
    out_weight = centred(keys[5], (ATT, D), ATT ** -0.5, 0.1875)
    mix_gain = jnp.clip(1.0 + 0.18 * jax.random.normal(keys[6], (D,), jnp.float32), 0.1, 1.9)
    ffn_gain = jnp.clip(1.0 + 0.18 * jax.random.normal(keys[7], (D,), jnp.float32), 0.1, 1.9)
    expert_ids_keys = jax.random.split(jax.random.fold_in(keys[8], 1), SEQUENCE_COUNT * SEQUENCE_LENGTH // TOK_DEV)
    expert_ids_turns = jax.random.permutation(jax.random.fold_in(keys[8], 3), SEQUENCE_COUNT * SEQUENCE_LENGTH // TOK_DEV)
    expert_ids = jax.vmap(lambda own, number: assign_block(jax.random.fold_in(keys[8], 2), own, number, TOK_DEV, EXPERTS, TOPK, CAP, 2))(expert_ids_keys, expert_ids_turns).reshape((SEQUENCE_COUNT, SEQUENCE_LENGTH, TOPK))
    route_weights = jnp.clip(jnp.exp(math.log(2.0) - 1.89712 * jax.random.uniform(keys[9], (SEQUENCE_COUNT, SEQUENCE_LENGTH, TOPK), jnp.float32) ** block_scale(keys[9], (SEQUENCE_COUNT, SEQUENCE_LENGTH, TOPK), ((0, 8), (1, 16)), -0.2, 0.2)), 0.3, 2.0)
    expert_gate = centred(keys[10], (EXPERTS, D, EFF), D ** -0.5, 0.125, ((0, 128),))
    expert_up = centred(keys[11], (EXPERTS, D, EFF), D ** -0.5, 0.125, ((0, 128),))
    expert_down = centred(keys[12], (EXPERTS, EFF, D), EFF ** -0.5, 0.25, ((0, 128),))
    shared_gate = centred(keys[13], (D, EFF), D ** -0.5, 0.125)
    shared_up = centred(keys[14], (D, EFF), D ** -0.5, 0.125)
    shared_down = centred(keys[15], (EFF, D), EFF ** -0.5, 0.25)
    return dict(residual_in=residual_in, query_rows=query_rows, key_rows=key_rows, value_rows=value_rows, gate_sums=gate_sums, out_weight=out_weight, mix_gain=mix_gain, ffn_gain=ffn_gain, expert_ids=expert_ids, route_weights=route_weights, expert_gate=expert_gate, expert_up=expert_up, expert_down=expert_down, shared_gate=shared_gate, shared_up=shared_up, shared_down=shared_down)


def reference(residual_in, query_rows, key_rows, value_rows, gate_sums, out_weight, mix_gain, ffn_gain, expert_ids, route_weights, expert_gate, expert_up, expert_down, shared_gate, shared_up, shared_down):
    score_scale = HEAD_DIM ** (-0.5)

    def one_head(pair_index):
        seq_index = pair_index // HEADS
        head_index = pair_index % HEADS
        zero = jnp.zeros((), jnp.int32)
        query_head = lax.dynamic_slice(query_rows, (seq_index, zero, head_index * HEAD_DIM), (1, SEQUENCE_LENGTH, HEAD_DIM))[0]
        key_head = lax.dynamic_slice(key_rows, (seq_index, zero, head_index * HEAD_DIM), (1, SEQUENCE_LENGTH, HEAD_DIM))[0]
        value_head = lax.dynamic_slice(value_rows, (seq_index, zero, head_index * HEAD_DIM), (1, SEQUENCE_LENGTH, HEAD_DIM))[0]
        sums_head = lax.dynamic_slice(gate_sums, (seq_index, head_index, zero), (1, 1, SEQUENCE_LENGTH))[0, 0]
        scores = jnp.dot(query_head, key_head.T, preferred_element_type=jnp.float32) * score_scale
        scores = scores + sums_head[:, None] - sums_head[None, :]
        causal_mask = jnp.arange(SEQUENCE_LENGTH)[None, :] <= jnp.arange(SEQUENCE_LENGTH)[:, None]
        scores = jnp.where(causal_mask, scores, -jnp.inf)
        peak = lax.optimization_barrier(jnp.max(scores, axis=1, keepdims=True))
        weights = jnp.exp(scores - peak)
        weights = (weights / lax.optimization_barrier(jnp.sum(weights, axis=1, keepdims=True))).astype(jnp.bfloat16)
        return jnp.dot(weights, value_head, preferred_element_type=jnp.float32).astype(jnp.bfloat16)
    heads_all = lax.map(one_head, jnp.arange(SEQUENCE_COUNT * HEADS, dtype=jnp.int32))
    heads_out = heads_all.reshape(SEQUENCE_COUNT, HEADS, SEQUENCE_LENGTH, HEAD_DIM).transpose(0, 2, 1, 3).reshape(SEQUENCE_COUNT * SEQUENCE_LENGTH, ATT)
    projected = jnp.dot(heads_out, out_weight, preferred_element_type=jnp.float32)
    residual_f = residual_in.reshape(SEQUENCE_COUNT * SEQUENCE_LENGTH, D).astype(jnp.float32)
    mixed_rows = residual_f + mix_gain * projected * lax.rsqrt(lax.optimization_barrier(jnp.mean(projected * projected, axis=1, keepdims=True)) + 1e-06)
    normed = (ffn_gain * mixed_rows * lax.rsqrt(lax.optimization_barrier(jnp.mean(mixed_rows * mixed_rows, axis=1, keepdims=True)) + 1e-06)).astype(jnp.bfloat16)
    gate_part = jnp.dot(normed, shared_gate, preferred_element_type=jnp.float32)
    up_part = jnp.dot(normed, shared_up, preferred_element_type=jnp.float32)
    shared_hidden = (jax.nn.silu(gate_part) * up_part).astype(jnp.bfloat16)
    shared_out = jnp.dot(shared_hidden, shared_down, preferred_element_type=jnp.float32)
    tokens_all = SEQUENCE_COUNT * SEQUENCE_LENGTH
    pair_total = tokens_all * TOPK
    sources = tokens_all // TOK_DEV
    per_source = TOK_DEV * TOPK
    id_blocks = expert_ids.reshape(sources, per_source)
    one_hot = (id_blocks[:, :, None] == jnp.arange(EXPERTS, dtype=jnp.int32)[None, None, :]).astype(jnp.int32)
    position_in = lax.optimization_barrier(jnp.sum((jnp.cumsum(one_hot, axis=1) - one_hot) * one_hot, axis=2))
    columns = jnp.arange(sources, dtype=jnp.int32)[:, None] * CAP + position_in
    pair_ids = jnp.arange(pair_total, dtype=jnp.int32).reshape(sources, per_source)
    table = jnp.full((EXPERTS, sources * CAP), pair_total, jnp.int32).at[id_blocks, columns].set(pair_ids)
    flat_weights = route_weights.reshape(pair_total)

    def one_expert(running, expert_index):
        pair_list = table[expert_index]
        is_valid = pair_list < pair_total
        token_list = jnp.where(is_valid, pair_list // TOPK, 0)
        weight_list = jnp.where(is_valid, flat_weights[jnp.minimum(pair_list, pair_total - 1)], 0.0)
        gathered = normed[token_list]
        gate_rows = jnp.dot(gathered, expert_gate[expert_index], preferred_element_type=jnp.float32)
        up_rows = jnp.dot(gathered, expert_up[expert_index], preferred_element_type=jnp.float32)
        hidden = (jax.nn.silu(gate_rows) * up_rows).astype(jnp.bfloat16)
        expert_out = jnp.dot(hidden, expert_down[expert_index], preferred_element_type=jnp.float32).astype(jnp.bfloat16)
        running = running.at[token_list].add(weight_list[:, None] * expert_out.astype(jnp.float32))
        return (running, None)
    routed, _ = lax.scan(one_expert, jnp.zeros((tokens_all, D), jnp.float32), jnp.arange(EXPERTS, dtype=jnp.int32))
    result_rows = (mixed_rows + shared_out + routed).astype(jnp.bfloat16)
    return result_rows.reshape(SEQUENCE_COUNT, SEQUENCE_LENGTH, D)
```

```python
import functools

import jax
import jax.numpy as jnp
from jax import lax
from jax.experimental import pallas as pl
from jax.experimental.pallas import tpu as pltpu
from jax.sharding import PartitionSpec as P

HEAD_DIM = 64
MESH = pl.DeviceIdType.MESH
PEERS = 128
SLOTS = 8
GROUPS = 4
PER = PEERS // GROUPS
F32 = jnp.float32
BF16 = jnp.bfloat16


def sent_together(arrays, axis, split_dim, concat_dim, along):
    both = jnp.concatenate(arrays, axis=along)
    out, at, gathered = (
        lax.all_to_all(both, axis, split_axis=split_dim, concat_axis=concat_dim, tiled=True),
        0,
        [],
    )
    for a in arrays:
        gathered.append(lax.slice_in_dim(out, at, at + a.shape[along], axis=along))
        at += a.shape[along]
    return tuple(gathered)


def attend(query_all, key_all, value_all, gate_sums):
    length = query_all.shape[1]
    head_count = gate_sums.shape[1]
    score_scale = HEAD_DIM ** (-0.5)
    query_heads = query_all[0].reshape(length, head_count, HEAD_DIM)
    key_heads = key_all[0].reshape(length, head_count, HEAD_DIM)
    value_heads = value_all[0].reshape(length, head_count, HEAD_DIM)
    sums_local = gate_sums[0]
    block_rows = min(512, length)
    pieces = []
    for block_index in range(length // block_rows):
        start = block_index * block_rows
        block_end = start + block_rows
        scores = (
            jnp.einsum(
                "qhd,khd->hqk",
                query_heads[start:block_end],
                key_heads[:block_end],
                preferred_element_type=jnp.float32,
            )
            * score_scale
        )
        scores = scores + sums_local[:, start:block_end, None] - sums_local[:, None, :block_end]
        causal_mask = jnp.arange(block_end)[None, :] <= jnp.arange(start, block_end)[:, None]
        scores = jnp.where(causal_mask[None], scores, -jnp.inf)
        peak = jnp.max(scores, axis=2, keepdims=True)
        weights = jnp.exp(scores - peak)
        weights = (weights / jnp.sum(weights, axis=2, keepdims=True)).astype(jnp.bfloat16)
        mixed_heads = jnp.einsum(
            "hqk,khd->qhd", weights, value_heads[:block_end], preferred_element_type=jnp.float32
        ).astype(jnp.bfloat16)
        pieces.append(mixed_heads.reshape(block_rows, head_count * HEAD_DIM))
    return jnp.concatenate(pieces, axis=0)[None]


def shift_of(k):
    group, core, dz, dx = k // 32, (k // 16) % 2, (k // 4) % 4, k % 4
    return dz, dx, (group + dz + dx) % 4, core


def moved(shift, sign):
    dz, dx, dy, dc = shift
    sp, dp = lax.axis_index("sp"), lax.axis_index("dp")
    z = (sp // 4 + sign * dz + 4) % 4
    x = (sp % 4 + sign * dx + 4) % 4
    y = (dp // 2 + sign * dy + 4) % 4
    c = (dp % 2 + dc) % 2
    return z * 4 + x, y * 2 + c


def dot(a, b):
    return jnp.dot(a, b, preferred_element_type=F32)


def moe_kernel(
    h_ref, res_ref, place_ref, mixw_ref, mixg_ref, ffng_ref,
    wo_any, sg_any, su_any, sd_any, eg_any, eu_any, ed_any,
    o_ref,
    wo, sg, su, sd, eg, eu, ed, outgoing, arrived, result, received, acc, normed,
    wsem, ready, out_s, out_r, ret_s, ret_r,
):
    loads = [
        pltpu.make_async_copy(src, dst, wsem.at[i])
        for i, (src, dst) in enumerate(
            [(wo_any, wo), (sg_any, sg), (su_any, su), (sd_any, sd), (eg_any, eg), (eu_any, eu), (ed_any, ed)]
        )
    ]
    for c in loads:
        c.start()
    barrier = pltpu.get_barrier_semaphore()

    def hello_sp(k, _):
        pl.semaphore_signal(barrier, inc=1, device_id=moved((k // 4, k % 4, 0, 0), 1), device_id_type=MESH)
        return 0

    def hello_dp(k, _):
        pl.semaphore_signal(barrier, inc=1, device_id=moved((0, 0, k // 2, k % 2), 1), device_id_type=MESH)
        return 0

    def row_ready(k, _):
        pl.semaphore_signal(ready, inc=1, device_id=moved((0, 0, k // 2, k % 2), 1), device_id_type=MESH)
        return 0

    lax.fori_loop(1, 16, hello_sp, 0)
    lax.fori_loop(1, 8, hello_dp, 0)

    loads[0].wait()
    projected = dot(h_ref[...], wo[...])
    pl.semaphore_wait(barrier, 22)
    lax.fori_loop(1, 8, row_ready, 0)
    mixed = res_ref[...].astype(F32) + mixg_ref[...] * projected * lax.rsqrt(
        jnp.mean(projected * projected, axis=1, keepdims=True) + 1e-06
    )
    acc[...] = mixed
    normed[...] = (
        ffng_ref[...] * mixed * lax.rsqrt(jnp.mean(mixed * mixed, axis=1, keepdims=True) + 1e-06)
    ).astype(BF16)
    pl.semaphore_wait(ready, 7)

    def out_copy(k, c):
        return pltpu.make_async_remote_copy(
            src_ref=outgoing.at[k], dst_ref=arrived.at[k], send_sem=out_s.at[c], recv_sem=out_r.at[c],
            device_id=moved(shift_of(k), 1), device_id_type=MESH,
        )

    def ret_copy(k, c):
        return pltpu.make_async_remote_copy(
            src_ref=result.at[k], dst_ref=received.at[k], send_sem=ret_s.at[c], recv_sem=ret_r.at[c],
            device_id=moved(shift_of(k), -1), device_id_type=MESH,
        )

    def send_group(copy, c):
        def one(k, _):
            copy(k, c).start()
            return 0

        lax.fori_loop(jnp.where(c == 0, 1, c * PER), (c + 1) * PER, one, 0)

    def wait_group(ref, sem, c):
        @pl.when(c == 0)
        def _():
            part = ref.at[pl.ds(1, PER - 1)]
            pltpu.make_async_copy(part, part, sem.at[0]).wait()

        @pl.when(c > 0)
        def _():
            part = ref.at[pl.ds(c * PER, PER)]
            pltpu.make_async_copy(part, part, sem.at[c]).wait()

    def pack(c, _):
        rows = dot(place_ref[pl.ds(pl.multiple_of(c * PER * SLOTS, PER * SLOTS), PER * SLOTS), :], normed[...])
        outgoing[pl.ds(c * PER, PER)] = rows.reshape(PER, SLOTS, rows.shape[1]).astype(BF16)

        @pl.when(c == 0)
        def _():
            arrived[0] = outgoing[0]

        send_group(out_copy, c)
        return 0

    lax.fori_loop(0, GROUPS, pack, 0)

    for c in loads[1:4]:
        c.wait()
    gate = dot(normed[...], sg[...])
    up = dot(normed[...], su[...])
    hidden = (gate / (1.0 + jnp.exp(-gate)) * up).astype(BF16)
    acc[...] += dot(hidden, sd[...])
    for c in loads[4:]:
        c.wait()

    def expert(c, _):
        wait_group(arrived, out_r, c)
        rows = arrived[pl.ds(c * PER, PER)].astype(F32).reshape(PER * SLOTS, arrived.shape[2]).astype(BF16)
        g = dot(rows, eg[...])
        u = dot(rows, eu[...])
        hid = (g / (1.0 + jnp.exp(-g)) * u).astype(BF16)
        y = dot(hid, ed[...])
        result[pl.ds(c * PER, PER)] = y.reshape(PER, SLOTS, y.shape[1]).astype(BF16)

        @pl.when(c == 0)
        def _():
            received[0] = result[0]

        send_group(ret_copy, c)
        return 0

    lax.fori_loop(0, GROUPS, expert, 0)

    def combine(c, _):
        wait_group(received, ret_r, c)
        rows = received[pl.ds(c * PER, PER)].astype(F32).reshape(PER * SLOTS, received.shape[2]).astype(BF16)
        w = mixw_ref[pl.ds(pl.multiple_of(c * PER * SLOTS, PER * SLOTS), PER * SLOTS), :]
        hi = w.astype(BF16)
        lo = (w - hi.astype(F32)).astype(BF16)
        dims = (((0,), (0,)), ((), ()))
        acc[...] += lax.dot_general(hi, rows, dims, preferred_element_type=F32) + lax.dot_general(
            lo, rows, dims, preferred_element_type=F32
        )
        return 0

    lax.fori_loop(0, GROUPS, combine, 0)
    o_ref[...] = acc[...].astype(BF16)

    def drain(c, _):
        wait_group(outgoing, out_s, c)
        wait_group(result, ret_s, c)
        return 0

    lax.fori_loop(0, GROUPS, drain, 0)


def moe_layer(heads, residual, place, mixw, mix_gain, ffn_gain, wo, sg, su, sd, eg, eu, ed):
    tok, width = residual.shape
    vm, hbm = pl.BlockSpec(memory_space=pltpu.VMEM), pl.BlockSpec(memory_space=pl.ANY)
    weights = (wo, sg, su, sd, eg, eu, ed)
    boxes = pltpu.VMEM((PEERS, SLOTS, width), BF16)
    return pl.pallas_call(
        moe_kernel,
        out_shape=jax.ShapeDtypeStruct((tok, width), BF16),
        in_specs=[vm] * 6 + [hbm] * 7,
        out_specs=vm,
        scratch_shapes=[pltpu.VMEM(w.shape, w.dtype) for w in weights]
        + [boxes] * 4
        + [pltpu.VMEM((tok, width), F32), pltpu.VMEM((tok, width), BF16)]
        + [pltpu.SemaphoreType.DMA((7,)), pltpu.SemaphoreType.REGULAR]
        + [pltpu.SemaphoreType.DMA((GROUPS,))] * 4,
        compiler_params=pltpu.CompilerParams(
            collective_id=1, has_side_effects=True, vmem_limit_bytes=60 * 2**20
        ),
        name="moe_layer",
    )(heads, residual, place, mixw, mix_gain[None], ffn_gain[None], *weights)


def routing(expert_ids, route_weights):
    tok, top = expert_ids.shape
    sp, dp = moved(shift_of(jnp.arange(PEERS, dtype=jnp.int32)), 1)
    peer = sp * 8 + dp
    hit = expert_ids.T[:, None, :] == peer[None, :, None]
    named = jnp.any(hit, axis=0)
    weight = jnp.sum(jnp.where(hit, route_weights.T[:, None, :], 0.0), axis=0)
    earlier = jnp.arange(tok)[:, None] < jnp.arange(tok)[None, :]
    rank = jnp.dot(named.astype(BF16), earlier.astype(BF16), preferred_element_type=F32).astype(jnp.int32)
    at = named[:, None, :] & (rank[:, None, :] == jnp.arange(SLOTS, dtype=jnp.int32)[None, :, None])
    place = at.astype(BF16).reshape(PEERS * SLOTS, tok)
    mixw = jnp.where(at, weight[:, None, :], 0.0).reshape(PEERS * SLOTS, tok)
    return place, mixw


def shards(
    residual_in,
    query_rows,
    key_rows,
    value_rows,
    gate_sums,
    out_weight,
    mix_gain,
    ffn_gain,
    expert_ids,
    route_weights,
    expert_gate,
    expert_up,
    expert_down,
    shared_gate,
    shared_up,
    shared_down,
):
    place, mixw = routing(expert_ids[0], route_weights[0])
    key_all, value_all = sent_together((key_rows, value_rows), "sp", 2, 1, 0)
    query_all = lax.all_to_all(query_rows, "sp", split_axis=2, concat_axis=1, tiled=True)
    attended = attend(query_all, key_all, value_all, gate_sums)
    returned = lax.all_to_all(attended, "sp", split_axis=1, concat_axis=2, tiled=True)
    return moe_layer(
        returned[0], residual_in[0], place, mixw, mix_gain, ffn_gain, out_weight,
        shared_gate, shared_up, shared_down, expert_gate[0], expert_up[0], expert_down[0],
    )[None]


def solution(mesh):
    return jax.shard_map(
        shards,
        mesh=mesh,
        in_specs=(
            P("dp", "sp", None),
            P("dp", "sp", None),
            P("dp", "sp", None),
            P("dp", "sp", None),
            P("dp", "sp", None),
            P(),
            P(),
            P(),
            P("dp", "sp", None),
            P("dp", "sp", None),
            P(("sp", "dp"), None, None),
            P(("sp", "dp"), None, None),
            P(("sp", "dp"), None, None),
            P(),
            P(),
            P(),
        ),
        out_specs=P("dp", "sp", None),
        check_vma=False,
    )
```

```python
import jax
import jax.numpy as jnp
from jax import lax
from jax.experimental import pallas as pl
from jax.experimental.pallas import tpu as pltpu
from jax.sharding import PartitionSpec as P

HEAD_DIM = 64
MESH = pl.DeviceIdType.MESH
PEERS = 128
SLOTS = 8
GROUPS = 4
PER = PEERS // GROUPS
F32 = jnp.float32
BF16 = jnp.bfloat16


def shift_of(k):
    group, core, dz, dx = k // 32, (k // 16) % 2, (k // 4) % 4, k % 4
    return dz, dx, (group + dz + dx) % 4, core


def moved(shift, sign):
    dz, dx, dy, dc = shift
    sp, dp = lax.axis_index("sp"), lax.axis_index("dp")
    z = (sp // 4 + sign * dz + 4) % 4
    x = (sp % 4 + sign * dx + 4) % 4
    y = (dp // 2 + sign * dy + 4) % 4
    c = (dp % 2 + dc) % 2
    return z * 4 + x, y * 2 + c


def dot(a, b):
    return jnp.dot(a, b, preferred_element_type=F32)


def swap_matrix():
    r = lax.broadcasted_iota(jnp.int32, (256, 256), 0)
    c = lax.broadcasted_iota(jnp.int32, (256, 256), 1)
    from_row = jnp.where((c >= 64) & (c < 128), c + 64, jnp.where((c >= 128) & (c < 192), c - 64, c))
    return jnp.where(r == from_row, 1.0, 0.0).astype(BF16)


def lifted(pairs):
    r = lax.broadcasted_iota(jnp.int32, (128, 256), 0)
    c = lax.broadcasted_iota(jnp.int32, (128, 256), 1)
    out = jnp.zeros((128, 256), F32)
    for row, col, scale in pairs:
        out = jnp.where((c >= col) & (c < col + 64) & (r - row == c - col), scale, out)
    return out.astype(BF16)


def layer_kernel(
    q_ref, k_ref, v_ref, gate_ref, ids_ref, rw_ref, res_ref, mixg_ref, ffng_ref,
    wo_any, sg_any, su_any, sd_any, eg_any, eu_any, ed_any,
    o_ref,
    wo, sg, su, sd, eg, eu, ed, outgoing, arrived, result, received, acc, normed,
    qkv_out, qkv_in, q_all, k_all, v_all, scores, att_out, heads_in, heads, code, weight,
    wsem, ready, out_s, out_r, ret_s, ret_r, qkv_s, qkv_r, att_s, att_r,
):
    loads = [
        pltpu.make_async_copy(src, dst, wsem.at[i])
        for i, (src, dst) in enumerate(
            [(wo_any, wo), (sg_any, sg), (su_any, su), (sd_any, sd), (eg_any, eg), (eu_any, eu), (ed_any, ed)]
        )
    ]
    me = lax.axis_index("sp")
    barrier = pltpu.get_barrier_semaphore()

    def hello_sp(k, _):
        pl.semaphore_signal(barrier, inc=1, device_id=moved((k // 4, k % 4, 0, 0), 1), device_id_type=MESH)
        return 0

    def hello_dp(k, _):
        pl.semaphore_signal(barrier, inc=1, device_id=moved((0, 0, k // 2, k % 2), 1), device_id_type=MESH)
        return 0

    def row_ready(k, _):
        pl.semaphore_signal(ready, inc=1, device_id=moved((0, 0, k // 2, k % 2), 1), device_id_type=MESH)
        return 0

    lax.fori_loop(1, 16, hello_sp, 0)
    lax.fori_loop(1, 8, hello_dp, 0)
    for c in loads:
        c.start()

    swap = swap_matrix()
    for p in range(8):
        cols = slice(p * 128, (p + 1) * 128)
        qk = dot(jnp.concatenate([q_ref[:, cols], k_ref[:, cols]], axis=1), swap).astype(BF16)
        vv = dot(jnp.concatenate([v_ref[:64, cols], v_ref[64:, cols]], axis=1), swap).astype(BF16)
        for side in range(2):
            part = slice(side * 128, (side + 1) * 128)
            qkv_out[2 * p + side, :128, :] = qk[:, part]
            qkv_out[2 * p + side, 128:, :] = vv[:, part]
    qkv_in[me] = qkv_out[me]

    pl.semaphore_wait(barrier, 22)

    def send_qkv(k, _):
        to = moved((k // 4, k % 4, 0, 0), 1)
        pltpu.make_async_remote_copy(
            src_ref=qkv_out.at[to[0]], dst_ref=qkv_in.at[me], send_sem=qkv_s, recv_sem=qkv_r,
            device_id=to, device_id_type=MESH,
        ).start()
        return 0

    lax.fori_loop(1, 16, send_qkv, 0)

    kth = lax.broadcasted_iota(jnp.int32, (PEERS, 1), 0)
    dz, dx = (kth >> 2) & 3, kth & 3
    dy, dc = ((kth >> 5) + dz + dx) & 3, (kth >> 4) & 1
    dp = lax.axis_index("dp")
    peer = (
        (((me // 4 + dz) & 3) * 4 + ((me % 4 + dx) & 3)) * 8 + ((dp // 2 + dy) & 3) * 2 + ((dp % 2 + dc) & 1)
    )
    named = jnp.zeros((PEERS, PEERS), F32)
    share = jnp.zeros((PEERS, PEERS), F32)
    for j in range(ids_ref.shape[0]):
        hit = ids_ref[j : j + 1, :] == peer
        named = jnp.where(hit, 1.0, named)
        share = jnp.where(hit, rw_ref[j : j + 1, :], share)
    earlier = jnp.where(
        lax.broadcasted_iota(jnp.int32, (PEERS, PEERS), 0) < lax.broadcasted_iota(jnp.int32, (PEERS, PEERS), 1),
        1.0,
        0.0,
    ).astype(BF16)
    rank = dot(named.astype(BF16), earlier)
    code[...] = jnp.where(named > 0.5, rank, -1.0)
    weight[...] = share

    pltpu.make_async_copy(qkv_in.at[pl.ds(0, 15)], qkv_in.at[pl.ds(0, 15)], qkv_r).wait()

    split_qk = lifted([(0, 0, HEAD_DIM**-0.5), (64, 128, 1.0)])
    split_v = lifted([(0, 0, 1.0), (0, 64, 1.0), (64, 128, 1.0), (64, 192, 1.0)])
    for j in range(16):
        rows = slice(j * 128, (j + 1) * 128)
        qk = dot(qkv_in[j, :128, :], split_qk).astype(BF16)
        vv = dot(qkv_in[j, 128:, :], split_v).astype(BF16)
        q_all[rows, :] = qk[:, :128]
        k_all[rows, :] = qk[:, 128:]
        v_all[j * 128 : j * 128 + 64, :] = vv[:, :128]
        v_all[j * 128 + 64 : (j + 1) * 128, :] = vv[:, 128:]

    left = lax.broadcasted_iota(jnp.int32, (64, 128), 1) < 64
    ahead = lax.broadcasted_iota(jnp.int32, (256, 256), 1) - lax.broadcasted_iota(jnp.int32, (256, 256), 0)

    def att_copy(b):
        return pltpu.make_async_remote_copy(
            src_ref=att_out.at[b], dst_ref=heads_in.at[me], send_sem=att_s, recv_sem=att_r,
            device_id=(b, lax.axis_index("dp")), device_id_type=MESH,
        )

    def attend(step, _):
        turn = (me // 2 + step) % 8
        q = q_all[pl.ds(pl.multiple_of(turn * 256, 256), 256), :]
        for group in range(4):

            @pl.when(turn // 2 == group)
            def _():
                last = group * 512
                parts = [slice(c, c + 256) for c in range(0, last + 512, 256)]
                base = gate_ref[:, last : last + 1]
                top = None
                for part in parts:
                    s = lax.dot_general(
                        q, k_all[part, :], (((1,), (1,)), ((), ())), preferred_element_type=F32
                    ) + (base - gate_ref[:, part])
                    if part.start >= last:
                        s = jnp.where(ahead <= (turn % 2) * 256 - (part.start - last), s, -jnp.inf)
                    scores[:, part] = s
                    peak = jnp.maximum(s[:, :128], s[:, 128:])
                    top = peak if top is None else jnp.maximum(top, peak)
                top = jnp.max(top, axis=1, keepdims=True)
                total = None
                for part in parts:
                    e = jnp.exp(scores[:, part] - top)
                    scores[:, part] = e
                    both = e[:, :128] + e[:, 128:]
                    total = both if total is None else total + both
                inverse = 1.0 / jnp.sum(total, axis=1, keepdims=True)
                o = None
                for part in parts:
                    piece = dot((scores[:, part] * inverse).astype(BF16), v_all[part, :])
                    o = piece if o is None else o + piece
                o = o.astype(BF16)
                att_out[2 * turn] = jnp.where(left, o[:64], o[64:128])
                att_out[2 * turn + 1] = jnp.where(left, o[128:192], o[192:])

        for half in range(2):
            b = 2 * turn + half

            @pl.when(b != me)
            def _():
                att_copy(b).start()

            @pl.when(b == me)
            def _():
                heads_in[me] = att_out[me]

        return 0

    lax.fori_loop(0, 8, attend, 0)
    pltpu.make_async_copy(heads_in.at[pl.ds(0, 15)], heads_in.at[pl.ds(0, 15)], att_r).wait()
    lax.fori_loop(1, 8, row_ready, 0)
    for p in range(8):
        two = dot(jnp.concatenate([heads_in[2 * p], heads_in[2 * p + 1]], axis=1), swap).astype(BF16)
        heads[:64, p * 128 : (p + 1) * 128] = two[:, :128]
        heads[64:, p * 128 : (p + 1) * 128] = two[:, 128:]

    loads[0].wait()
    projected = dot(heads[...], wo[...])
    mixed = res_ref[...].astype(F32) + mixg_ref[...] * projected * lax.rsqrt(
        jnp.mean(projected * projected, axis=1, keepdims=True) + 1e-06
    )
    acc[...] = mixed
    normed[...] = (
        ffng_ref[...] * mixed * lax.rsqrt(jnp.mean(mixed * mixed, axis=1, keepdims=True) + 1e-06)
    ).astype(BF16)
    pl.semaphore_wait(ready, 7)

    def slots_of(values, c):
        part = pl.ds(pl.multiple_of(c * PER, PER), PER)
        r = lax.broadcasted_iota(jnp.int32, (PER, SLOTS, PEERS), 1).astype(F32)
        at = code[part, :][:, None, :] == r
        return jnp.where(at, values(part), 0.0).reshape(PER * SLOTS, PEERS)

    def out_copy(k, c):
        return pltpu.make_async_remote_copy(
            src_ref=outgoing.at[k], dst_ref=arrived.at[k], send_sem=out_s.at[c], recv_sem=out_r.at[c],
            device_id=moved(shift_of(k), 1), device_id_type=MESH,
        )

    def ret_copy(k, c):
        return pltpu.make_async_remote_copy(
            src_ref=result.at[k], dst_ref=received.at[k], send_sem=ret_s.at[c], recv_sem=ret_r.at[c],
            device_id=moved(shift_of(k), -1), device_id_type=MESH,
        )

    def send_group(copy, c):
        def one(k, _):
            copy(k, c).start()
            return 0

        lax.fori_loop(jnp.where(c == 0, 1, c * PER), (c + 1) * PER, one, 0)

    def wait_group(ref, sem, c):
        @pl.when(c == 0)
        def _():
            part = ref.at[pl.ds(1, PER - 1)]
            pltpu.make_async_copy(part, part, sem.at[0]).wait()

        @pl.when(c > 0)
        def _():
            part = ref.at[pl.ds(c * PER, PER)]
            pltpu.make_async_copy(part, part, sem.at[c]).wait()

    def pack(c, _):
        rows = dot(slots_of(lambda part: 1.0, c).astype(BF16), normed[...])
        outgoing[pl.ds(c * PER, PER)] = rows.reshape(PER, SLOTS, rows.shape[1]).astype(BF16)

        @pl.when(c == 0)
        def _():
            arrived[0] = outgoing[0]

        send_group(out_copy, c)
        return 0

    lax.fori_loop(0, GROUPS, pack, 0)

    for c in loads[1:4]:
        c.wait()
    gate = dot(normed[...], sg[...])
    up = dot(normed[...], su[...])
    hidden = (gate / (1.0 + jnp.exp(-gate)) * up).astype(BF16)
    acc[...] += dot(hidden, sd[...])
    for c in loads[4:]:
        c.wait()

    def expert(c, _):
        wait_group(arrived, out_r, c)
        rows = arrived[pl.ds(c * PER, PER)].astype(F32).reshape(PER * SLOTS, arrived.shape[2]).astype(BF16)
        g = dot(rows, eg[...])
        u = dot(rows, eu[...])
        hid = (g / (1.0 + jnp.exp(-g)) * u).astype(BF16)
        y = dot(hid, ed[...])
        result[pl.ds(c * PER, PER)] = y.reshape(PER, SLOTS, y.shape[1]).astype(BF16)

        @pl.when(c == 0)
        def _():
            received[0] = result[0]

        send_group(ret_copy, c)
        return 0

    lax.fori_loop(0, GROUPS, expert, 0)

    def combine(c, _):
        wait_group(received, ret_r, c)
        rows = received[pl.ds(c * PER, PER)].astype(F32).reshape(PER * SLOTS, received.shape[2]).astype(BF16)
        w = slots_of(lambda part: weight[part, :][:, None, :], c)
        hi = w.astype(BF16)
        lo = (w - hi.astype(F32)).astype(BF16)
        dims = (((0,), (0,)), ((), ()))
        acc[...] += lax.dot_general(hi, rows, dims, preferred_element_type=F32) + lax.dot_general(
            lo, rows, dims, preferred_element_type=F32
        )
        return 0

    lax.fori_loop(0, GROUPS, combine, 0)
    o_ref[...] = acc[...].astype(BF16)

    pltpu.make_async_copy(qkv_out.at[pl.ds(0, 15)], qkv_out.at[pl.ds(0, 15)], qkv_s).wait()
    pltpu.make_async_copy(att_out.at[pl.ds(0, 15)], att_out.at[pl.ds(0, 15)], att_s).wait()

    def drain(c, _):
        wait_group(outgoing, out_s, c)
        wait_group(result, ret_s, c)
        return 0

    lax.fori_loop(0, GROUPS, drain, 0)


def layer(q, k, v, gates, ids, rw, residual, mix_gain, ffn_gain, *weights):
    tok, width = residual.shape
    length = gates.shape[1]
    vm, hbm = pl.BlockSpec(memory_space=pltpu.VMEM), pl.BlockSpec(memory_space=pl.ANY)
    boxes = pltpu.VMEM((PEERS, SLOTS, width), BF16)
    dma, dma_groups = pltpu.SemaphoreType.DMA, pltpu.SemaphoreType.DMA((GROUPS,))
    return pl.pallas_call(
        layer_kernel,
        out_shape=jax.ShapeDtypeStruct((tok, width), BF16),
        in_specs=[vm] * 9 + [hbm] * 7,
        out_specs=vm,
        scratch_shapes=[pltpu.VMEM(w.shape, w.dtype) for w in weights]
        + [boxes] * 4
        + [pltpu.VMEM((tok, width), F32), pltpu.VMEM((tok, width), BF16)]
        + [pltpu.VMEM((16, 192, 128), BF16)] * 2
        + [pltpu.VMEM((length, 128), BF16)] * 3
        + [pltpu.VMEM((256, length), F32)]
        + [pltpu.VMEM((16, 64, 128), BF16)] * 2
        + [pltpu.VMEM((tok, 1024), BF16)]
        + [pltpu.VMEM((PEERS, PEERS), F32)] * 2
        + [dma((7,)), pltpu.SemaphoreType.REGULAR]
        + [dma_groups] * 4
        + [dma] * 4,
        compiler_params=pltpu.CompilerParams(
            collective_id=1, has_side_effects=True, vmem_limit_bytes=60 * 2**20
        ),
        name="layer",
    )(q, k, v, gates, ids, rw, residual, mix_gain[None], ffn_gain[None], *weights)


def shards(
    residual_in,
    query_rows,
    key_rows,
    value_rows,
    gate_sums,
    out_weight,
    mix_gain,
    ffn_gain,
    expert_ids,
    route_weights,
    expert_gate,
    expert_up,
    expert_down,
    shared_gate,
    shared_up,
    shared_down,
):
    return layer(
        query_rows[0], key_rows[0], value_rows[0], gate_sums[0], expert_ids[0].T, route_weights[0].T,
        residual_in[0], mix_gain, ffn_gain, out_weight,
        shared_gate, shared_up, shared_down, expert_gate[0], expert_up[0], expert_down[0],
    )[None]


def solution(mesh):
    return jax.shard_map(
        shards,
        mesh=mesh,
        in_specs=(
            P("dp", "sp", None),
            P("dp", "sp", None),
            P("dp", "sp", None),
            P("dp", "sp", None),
            P("dp", "sp", None),
            P(),
            P(),
            P(),
            P("dp", "sp", None),
            P("dp", "sp", None),
            P(("sp", "dp"), None, None),
            P(("sp", "dp"), None, None),
            P(("sp", "dp"), None, None),
            P(),
            P(),
            P(),
        ),
        out_specs=P("dp", "sp", None),
        check_vma=False,
    )
```

```python
import jax
import jax.numpy as jnp
from jax import lax
from jax.experimental import pallas as pl
from jax.experimental.pallas import tpu as pltpu
from jax.sharding import PartitionSpec as P

HEAD_DIM = 64
MESH = pl.DeviceIdType.MESH
PEERS = 128
SLOTS = 8
GROUPS = 4
PER = PEERS // GROUPS
CUTS = (slice(0, 768), slice(768, 1408), slice(1408, 2048))
F32 = jnp.float32
BF16 = jnp.bfloat16


class Torus:
    def __init__(self):
        sp, dp = lax.axis_index("sp"), lax.axis_index("dp")
        self.z, self.x, self.y, self.c = sp // 4, sp % 4, dp // 2, dp % 2
        zs = [(self.z + d) % 4 for d in range(4)]
        self.xs = [(self.x + d) % 4 for d in range(4)]
        self.ys = [(self.y + d) % 4 for d in range(4)]
        cs = [self.c, 1 - self.c]
        self.sp = [[zs[dz] * 4 + self.xs[dx] for dx in range(4)] for dz in range(4)]
        self.dp = [[self.ys[dy] * 2 + cs[dc] for dc in range(2)] for dy in range(4)]

    def at(self, dz, dx, dy, dc):
        return self.sp[dz % 4][dx % 4], self.dp[dy % 4][dc]

    def along(self, axis, d):
        return self.at(*[d if a == axis else 0 for a in range(3)], 0)

    def back(self, dz, dx, dy, dc):
        return self.sp[-dz % 4][-dx % 4], self.ys[-dy % 4] * 2 + (self.c + dc) % 2


def lane_of(axis, d, dc, a, b):
    place = [a, b]
    place.insert(axis, d)
    if isinstance(place[0], int):
        place[0] = swapped(place[0])
    return (dc, *place)


def swapped(i):
    return i % 2 * 2 + i // 2


def dot(a, b):
    return jnp.dot(a, b, preferred_element_type=F32)


def swap_matrix():
    r = lax.broadcasted_iota(jnp.int32, (256, 256), 0)
    c = lax.broadcasted_iota(jnp.int32, (256, 256), 1)
    from_row = jnp.where((c >= 64) & (c < 128), c + 64, jnp.where((c >= 128) & (c < 192), c - 64, c))
    return jnp.where(r == from_row, 1.0, 0.0).astype(BF16)


def lifted(pairs):
    r = lax.broadcasted_iota(jnp.int32, (128, 256), 0)
    c = lax.broadcasted_iota(jnp.int32, (128, 256), 1)
    out = jnp.zeros((128, 256), F32)
    for row, col, scale in pairs:
        out = jnp.where((c >= col) & (c < col + 64) & (r - row == c - col), scale, out)
    return out.astype(BF16)


def layer_kernel(
    q_ref, k_ref, v_ref, gate_ref, info_ref, res_ref, mixg_ref, ffng_ref,
    wo_any, sg_any, su_any, sd_any, eg_any, eu_any, ed_any,
    o_ref,
    wo, sg, su, sd, eg, eu, ed, outgoing, arrived, result, received, acc, normed,
    qkv_out, qkv_in, q_all, k_all, v_all, scores, att_out, heads_in, heads, info, pack_code, pack_weight, ag_z, ag_x, ag_y,
    send_z, send_x, send_y, get_z, get_x, get_y,
    wsem, ready, out_s, out_r, ret_s, ret_r, qkv_s, qkv_r, att_s, att_r, info_s, info_r, ag_s, ag_r, part_s, part_r,
):
    loads = [
        pltpu.make_async_copy(src, dst, wsem.at[i])
        for i, (src, dst) in enumerate(
            [(wo_any, wo), (sg_any, sg), (su_any, su), (sd_any, sd), (eg_any, eg), (eu_any, eu), (ed_any, ed)]
        )
    ]
    me = lax.axis_index("sp")
    barrier = pltpu.get_barrier_semaphore()

    torus = Torus()
    dp = lax.axis_index("dp")
    row = [torus.sp[k // 4][k % 4] for k in range(1, 16)]
    column = [torus.dp[k // 2][k % 2] for k in range(1, 8)]
    for to in row:
        pl.semaphore_signal(barrier, inc=1, device_id=(to, dp), device_id_type=MESH)
    for to in column:
        pl.semaphore_signal(barrier, inc=1, device_id=(me, to), device_id_type=MESH)
    for c in loads:
        c.start()

    swap = swap_matrix()
    for p in range(8):
        cols = slice(p * 128, (p + 1) * 128)
        qk = dot(jnp.concatenate([q_ref[:, cols], k_ref[:, cols]], axis=1), swap).astype(BF16)
        vv = dot(jnp.concatenate([v_ref[:64, cols], v_ref[64:, cols]], axis=1), swap).astype(BF16)
        for side in range(2):
            part = slice(side * 128, (side + 1) * 128)
            qkv_out[2 * p + side, :128, :] = qk[:, part]
            qkv_out[2 * p + side, 128:, :] = vv[:, part]
    qkv_in[me] = qkv_out[me]

    pl.semaphore_wait(barrier, 22)

    for to in row:
        pltpu.make_async_remote_copy(
            src_ref=qkv_out.at[to], dst_ref=qkv_in.at[me], send_sem=qkv_s, recv_sem=qkv_r,
            device_id=(to, dp), device_id_type=MESH,
        ).start()

    def info_copy(axis, d):
        return pltpu.make_async_remote_copy(
            src_ref=info_ref, dst_ref=info.at[axis * 3 + d - 1], send_sem=info_s, recv_sem=info_r,
            device_id=torus.along(axis, d), device_id_type=MESH,
        )

    for axis in range(3):
        for d in range(1, 4):
            info_copy(axis, d).start()

    def expert_at(dz, dx, dy, dc):
        return (((torus.z + dz) & 3) * 4 + ((torus.x + dx) & 3)) * 8 + ((torus.y + dy) & 3) * 2 + ((torus.c + dc) & 1)

    earlier = jnp.where(
        lax.broadcasted_iota(jnp.int32, (PEERS, PEERS), 0) < lax.broadcasted_iota(jnp.int32, (PEERS, PEERS), 1),
        1.0,
        0.0,
    ).astype(BF16)

    def named_in(rows, peer):
        named = jnp.zeros((peer.shape[0], PEERS), F32)
        share = jnp.zeros((peer.shape[0], PEERS), F32)
        for j in range(4):
            hit = rows[j : j + 1, :] == peer
            named = jnp.where(hit, 1.0, named)
            share = jnp.where(hit, rows[4 + j : 5 + j, :], share)
        return named, share

    def ranked(named):
        return jnp.where(named > 0.5, dot(named.astype(BF16), earlier), -1.0)

    jth = lax.broadcasted_iota(jnp.int32, (PER, 1), 0)
    jc, ja, jb = jth >> 4, (jth >> 2) & 3, jth & 3
    js = (ja & 1) * 2 + (ja >> 1)
    planes = [expert_at(0, ja, jb, jc), expert_at(js, 0, jb, jc), expert_at(js, jb, 0, jc)]
    planes = [p.astype(F32) for p in planes]
    pltpu.make_async_copy(info, info, info_r).wait()
    for axis in range(3):
        parts = [named_in(info_ref[...], planes[axis])]
        for d in range(1, 4):
            parts.append(named_in(info[axis * 3 + d - 1], planes[axis]))
        pack_code[axis] = ranked(jnp.concatenate([p[0] for p in parts], axis=0))
        pack_weight[axis] = jnp.concatenate([p[1] for p in parts], axis=0)

    pltpu.make_async_copy(qkv_in.at[pl.ds(0, 15)], qkv_in.at[pl.ds(0, 15)], qkv_r).wait()

    split_qk = lifted([(0, 0, HEAD_DIM**-0.5), (64, 128, 1.0)])
    split_v = lifted([(0, 0, 1.0), (0, 64, 1.0), (64, 128, 1.0), (64, 192, 1.0)])
    for j in range(16):
        rows = slice(j * 128, (j + 1) * 128)
        qk = dot(qkv_in[j, :128, :], split_qk).astype(BF16)
        vv = dot(qkv_in[j, 128:, :], split_v).astype(BF16)
        q_all[rows, :] = qk[:, :128]
        k_all[rows, :] = qk[:, 128:]
        v_all[j * 128 : j * 128 + 64, :] = vv[:, :128]
        v_all[j * 128 + 64 : (j + 1) * 128, :] = vv[:, 128:]

    left = lax.broadcasted_iota(jnp.int32, (64, 128), 1) < 64
    ahead = lax.broadcasted_iota(jnp.int32, (256, 256), 1) - lax.broadcasted_iota(jnp.int32, (256, 256), 0)

    def att_copy(b):
        return pltpu.make_async_remote_copy(
            src_ref=att_out.at[b], dst_ref=heads_in.at[me], send_sem=att_s, recv_sem=att_r,
            device_id=(b, dp), device_id_type=MESH,
        )

    def attend(step, _):
        turn = (me // 2 + step) % 8
        q = q_all[pl.ds(pl.multiple_of(turn * 256, 256), 256), :]
        for group in range(4):

            @pl.when(turn // 2 == group)
            def _():
                last = group * 512
                parts = [slice(c, c + 256) for c in range(0, last + 512, 256)]
                base = gate_ref[:, last : last + 1]
                top = None
                for part in parts:
                    s = lax.dot_general(
                        q, k_all[part, :], (((1,), (1,)), ((), ())), preferred_element_type=F32
                    ) + (base - gate_ref[:, part])
                    if part.start >= last:
                        s = jnp.where(ahead <= (turn % 2) * 256 - (part.start - last), s, -jnp.inf)
                    scores[:, part] = s
                    peak = jnp.maximum(s[:, :128], s[:, 128:])
                    top = peak if top is None else jnp.maximum(top, peak)
                top = jnp.max(top, axis=1, keepdims=True)
                total = None
                for part in parts:
                    e = jnp.exp(scores[:, part] - top)
                    scores[:, part] = e
                    both = e[:, :128] + e[:, 128:]
                    total = both if total is None else total + both
                inverse = 1.0 / jnp.sum(total, axis=1, keepdims=True)
                o = None
                for part in parts:
                    piece = dot((scores[:, part] * inverse).astype(BF16), v_all[part, :])
                    o = piece if o is None else o + piece
                o = o.astype(BF16)
                att_out[2 * turn] = jnp.where(left, o[:64], o[64:128])
                att_out[2 * turn + 1] = jnp.where(left, o[128:192], o[192:])

        for half in range(2):
            b = 2 * turn + half

            @pl.when(b != me)
            def _():
                att_copy(b).start()

            @pl.when(b == me)
            def _():
                heads_in[me] = att_out[me]

        return 0

    lax.fori_loop(0, 8, attend, 0)
    pltpu.make_async_copy(heads_in.at[pl.ds(0, 15)], heads_in.at[pl.ds(0, 15)], att_r).wait()
    for to in column:
        pl.semaphore_signal(ready, inc=1, device_id=(me, to), device_id_type=MESH)
    for p in range(8):
        two = dot(jnp.concatenate([heads_in[2 * p], heads_in[2 * p + 1]], axis=1), swap).astype(BF16)
        heads[:64, p * 128 : (p + 1) * 128] = two[:, :128]
        heads[64:, p * 128 : (p + 1) * 128] = two[:, 128:]

    loads[0].wait()
    projected = dot(heads[...], wo[...])
    mixed = res_ref[...].astype(F32) + mixg_ref[...] * projected * lax.rsqrt(
        jnp.mean(projected * projected, axis=1, keepdims=True) + 1e-06
    )
    acc[...] = mixed
    normed[...] = (
        ffng_ref[...] * mixed * lax.rsqrt(jnp.mean(mixed * mixed, axis=1, keepdims=True) + 1e-06)
    ).astype(BF16)
    pl.semaphore_wait(ready, 7)

    def slots_of(ranks, values):
        r = lax.broadcasted_iota(jnp.int32, (PER, SLOTS, PEERS), 1).astype(F32)
        return jnp.where(ranks[:, None, :] == r, values, 0.0).reshape(PER * SLOTS, PEERS)

    gathered = (ag_z, ag_x, ag_y)
    for axis in range(3):
        for d in range(1, 4):
            pltpu.make_async_remote_copy(
                src_ref=normed.at[:, CUTS[axis]], dst_ref=gathered[axis].at[d - 1], send_sem=ag_s.at[axis], recv_sem=ag_r.at[axis],
                device_id=torus.along(axis, d), device_id_type=MESH,
            ).start()

    def pack(axis, d):
        cut = CUTS[axis]
        source = normed[:, cut] if d == 0 else gathered[axis][d - 1]
        place = slots_of(pack_code[axis, d * PER : (d + 1) * PER, :], 1.0).astype(BF16)
        rows = dot(place, source)
        box = lane_of(axis, d, slice(None), slice(None), slice(None))
        outgoing[(*box, slice(None), cut)] = rows.reshape(2, 4, 4, SLOTS, rows.shape[1]).astype(BF16)

    def send_planes(d, axes, cores):
        for dc in cores:
            for m in range(16):
                for axis in axes:
                    a, b = m % 4, (m // 4 + m) % 4
                    if axis == 1:
                        a, b = b, a
                    box = (*lane_of(axis, d, dc, a, b), slice(None), CUTS[axis])
                    if (dc, a, b) == (0, 0, 0):
                        arrived[box] = outgoing[box]
                        continue
                    way = [a, b]
                    way.insert(axis, 0)
                    pltpu.make_async_remote_copy(
                        src_ref=outgoing.at[box], dst_ref=arrived.at[box],
                        send_sem=out_s.at[dc], recv_sem=out_r.at[dc],
                        device_id=torus.at(*way, dc), device_id_type=MESH,
                    ).start()

    for axis in range(3):
        pack(axis, 0)
    send_planes(0, range(3), (0, 1))
    for axis in range(3):
        pltpu.make_async_copy(gathered[axis], gathered[axis], ag_r.at[axis]).wait()
        for d in range(1, 4):
            pack(axis, d)
    send_planes(slice(1, 4), range(3), (0, 1))

    def taken(ref, sem, *boxes):
        for box in boxes:
            part = ref.at[box]
            pltpu.make_async_copy(part, part, sem).wait()

    def wait_planes(ref, sem, dc):
        @pl.when(dc == 0)
        def _():
            taken(ref, sem.at[0], (0, *[slice(None)] * 4, slice(0, 1920)))

        @pl.when(dc == 1)
        def _():
            taken(ref, sem.at[1], (1,))

    def wait_back(ref, sem, dc, own):
        whole, most = slice(None), slice(0, 1920)
        if dc == 0:
            box = (0, 0, whole, whole, whole, most) if own else (0, pl.ds(0, 3), whole, whole, whole, most)
        else:
            box = (1, 3) if own else (1, pl.ds(0, 3))
        taken(ref, sem.at[dc * 2 + own], box)

    def send_back(dc):
        for own, d in enumerate([slice(1, 4), 0]):
            for m in range(16):
                for axis in range(3):
                    a, b = m % 4, (m // 4 + m) % 4
                    if axis == 1:
                        a, b = b, a
                    box = (*lane_of(axis, d, dc, a, b), slice(None), CUTS[axis])
                    way = [a, b]
                    way.insert(axis, 0)

                    def remote():
                        pltpu.make_async_remote_copy(
                            src_ref=result.at[box], dst_ref=received.at[box],
                            send_sem=ret_s.at[dc * 2 + own], recv_sem=ret_r.at[dc * 2 + own],
                            device_id=torus.back(*way, dc), device_id_type=MESH,
                        ).start()

                    if (a, b) == (0, 0):

                        @pl.when(dc == 0)
                        def _():
                            received[box] = result[box]

                        pl.when(dc > 0)(remote)
                    else:
                        remote()

    def combined(axis, d):
        box = lane_of(axis, d, slice(None), slice(None), slice(None))
        rows = received[(*box, slice(None), CUTS[axis])]
        rows = rows.astype(F32).reshape(PER * SLOTS, rows.shape[4]).astype(BF16)
        part = slice(d * PER, (d + 1) * PER)
        w = slots_of(pack_code[axis, part, :], pack_weight[axis, part, :][:, None, :])
        hi = w.astype(BF16)
        lo = (w - hi.astype(F32)).astype(BF16)
        dims = (((0,), (0,)), ((), ()))
        return lax.dot_general(hi, rows, dims, preferred_element_type=F32) + lax.dot_general(
            lo, rows, dims, preferred_element_type=F32
        )

    for c in loads[1:4]:
        c.wait()
    gate = dot(normed[...], sg[...])
    up = dot(normed[...], su[...])
    hidden = (gate / (1.0 + jnp.exp(-gate)) * up).astype(BF16)
    acc[...] += dot(hidden, sd[...])
    for c in loads[4:]:
        c.wait()

    def expert(dc, h):
        here = (dc, pl.ds(h * 2, 2))
        rows = arrived[here].astype(F32).reshape(PER * SLOTS, arrived.shape[5]).astype(BF16)
        g = dot(rows, eg[...])
        u = dot(rows, eu[...])
        hid = (g / (1.0 + jnp.exp(-g)) * u).astype(BF16)
        y = dot(hid, ed[...])
        result[here] = y.reshape(2, 4, 4, SLOTS, y.shape[1]).astype(BF16)
        return dc

    def experts(dc, _):
        wait_planes(arrived, out_r, dc)
        lax.fori_loop(0, 2, lambda h, core: expert(core, h), dc)
        send_back(dc)
        return 0

    lax.fori_loop(0, 2, experts, 0)

    sends, gets = (send_z, send_x, send_y), (get_z, get_x, get_y)
    wait_back(received, ret_r, 0, 0)
    wait_back(received, ret_r, 0, 1)
    wait_back(received, ret_r, 1, 0)
    for axis in range(3):
        for d in range(1, 4):
            sends[axis][d - 1] = combined(axis, d).astype(BF16)
            pltpu.make_async_remote_copy(
                src_ref=sends[axis].at[d - 1], dst_ref=gets[axis].at[d - 1],
                send_sem=part_s.at[axis], recv_sem=part_r.at[axis],
                device_id=torus.along(axis, -d), device_id_type=MESH,
            ).start()
    wait_back(received, ret_r, 1, 1)
    for axis in range(3):
        acc[:, CUTS[axis]] += combined(axis, 0)
    for axis in range(3):
        pltpu.make_async_copy(gets[axis], gets[axis], part_r.at[axis]).wait()
        add = gets[axis][0].astype(F32) + gets[axis][1].astype(F32) + gets[axis][2].astype(F32)
        acc[:, CUTS[axis]] += add
    o_ref[...] = acc[...].astype(BF16)

    pltpu.make_async_copy(qkv_out.at[pl.ds(0, 15)], qkv_out.at[pl.ds(0, 15)], qkv_s).wait()
    pltpu.make_async_copy(att_out.at[pl.ds(0, 15)], att_out.at[pl.ds(0, 15)], att_s).wait()

    pltpu.make_async_copy(info, info, info_s).wait()
    for axis in range(3):
        pltpu.make_async_copy(gathered[axis], gathered[axis], ag_s.at[axis]).wait()
    for dc in range(2):
        wait_planes(outgoing, out_s, dc)

    for dc in range(2):
        for own in range(2):
            wait_back(result, ret_s, dc, own)
    for axis in range(3):
        pltpu.make_async_copy(sends[axis], sends[axis], part_s.at[axis]).wait()


def layer(q, k, v, gates, info, residual, mix_gain, ffn_gain, *weights):
    tok, width = residual.shape
    length = gates.shape[1]
    vm, hbm = pl.BlockSpec(memory_space=pltpu.VMEM), pl.BlockSpec(memory_space=pl.ANY)
    boxes = pltpu.VMEM((2, 4, 4, 4, SLOTS, width), BF16)
    dma, dma_groups = pltpu.SemaphoreType.DMA, pltpu.SemaphoreType.DMA((GROUPS,))
    return pl.pallas_call(
        layer_kernel,
        out_shape=jax.ShapeDtypeStruct((tok, width), BF16),
        in_specs=[vm] * 8 + [hbm] * 7,
        out_specs=vm,
        scratch_shapes=[pltpu.VMEM(w.shape, w.dtype) for w in weights]
        + [boxes] * 4
        + [pltpu.VMEM((tok, width), F32), pltpu.VMEM((tok, width), BF16)]
        + [pltpu.VMEM((16, 192, 128), BF16)] * 2
        + [pltpu.VMEM((length, 128), BF16)] * 3
        + [pltpu.VMEM((256, length), F32)]
        + [pltpu.VMEM((16, 64, 128), BF16)] * 2
        + [pltpu.VMEM((tok, 1024), BF16)]
        + [pltpu.VMEM((9, 8, tok), F32)]
        + [pltpu.VMEM((3, PEERS, PEERS), F32)] * 2
        + [pltpu.VMEM((3, tok, cut.stop - cut.start), BF16) for cut in CUTS] * 3
        + [dma((7,)), pltpu.SemaphoreType.REGULAR]
        + [pltpu.SemaphoreType.DMA((2,))] * 2
        + [dma_groups] * 2
        + [dma] * 6
        + [dma((3,))] * 4,
        compiler_params=pltpu.CompilerParams(
            collective_id=1, has_side_effects=True, vmem_limit_bytes=60 * 2**20
        ),
        name="layer",
    )(q, k, v, gates, info, residual, mix_gain[None], ffn_gain[None], *weights)


def shards(
    residual_in,
    query_rows,
    key_rows,
    value_rows,
    gate_sums,
    out_weight,
    mix_gain,
    ffn_gain,
    expert_ids,
    route_weights,
    expert_gate,
    expert_up,
    expert_down,
    shared_gate,
    shared_up,
    shared_down,
):
    info = jnp.concatenate([expert_ids[0].astype(F32), route_weights[0]], axis=1).T
    return layer(
        query_rows[0], key_rows[0], value_rows[0], gate_sums[0], info,
        residual_in[0], mix_gain, ffn_gain, out_weight,
        shared_gate, shared_up, shared_down, expert_gate[0], expert_up[0], expert_down[0],
    )[None]


def solution(mesh):
    return jax.shard_map(
        shards,
        mesh=mesh,
        in_specs=(
            P("dp", "sp", None),
            P("dp", "sp", None),
            P("dp", "sp", None),
            P("dp", "sp", None),
            P("dp", "sp", None),
            P(),
            P(),
            P(),
            P("dp", "sp", None),
            P("dp", "sp", None),
            P(("sp", "dp"), None, None),
            P(("sp", "dp"), None, None),
            P(("sp", "dp"), None, None),
            P(),
            P(),
            P(),
        ),
        out_specs=P("dp", "sp", None),
        check_vma=False,
    )
```

```python
import jax
import jax.numpy as jnp
from jax import lax
from jax.experimental import pallas as pl
from jax.experimental.pallas import tpu as pltpu
from jax.sharding import PartitionSpec as P

HEAD_DIM = 64
MESH = pl.DeviceIdType.MESH
PEERS = 128
SLOTS = 8
GROUPS = 4
PER = PEERS // GROUPS
CUTS = (slice(0, 768), slice(768, 1408), slice(1408, 2048))
F32 = jnp.float32
BF16 = jnp.bfloat16


class Torus:
    def __init__(self):
        sp, dp = lax.axis_index("sp"), lax.axis_index("dp")
        self.z, self.x, self.y, self.c = sp // 4, sp % 4, dp // 2, dp % 2
        zs = [(self.z + d) % 4 for d in range(4)]
        self.xs = [(self.x + d) % 4 for d in range(4)]
        self.ys = [(self.y + d) % 4 for d in range(4)]
        cs = [self.c, 1 - self.c]
        self.sp = [[zs[dz] * 4 + self.xs[dx] for dx in range(4)] for dz in range(4)]
        self.dp = [[self.ys[dy] * 2 + cs[dc] for dc in range(2)] for dy in range(4)]

    def at(self, dz, dx, dy, dc):
        return self.sp[dz % 4][dx % 4], self.dp[dy % 4][dc]

    def along(self, axis, d):
        return self.at(*[d if a == axis else 0 for a in range(3)], 0)

    def back(self, dz, dx, dy, dc):
        return self.sp[-dz % 4][-dx % 4], self.ys[-dy % 4] * 2 + (self.c + dc) % 2


def lane_of(axis, d, dc, a, b):
    place = [a, b]
    place.insert(axis, d)
    if isinstance(place[0], int):
        place[0] = swapped(place[0])
    return (dc, *place)


def swapped(i):
    return i % 2 * 2 + i // 2


def dot(a, b):
    return jnp.dot(a, b, preferred_element_type=F32)


def swap_matrix():
    r = lax.broadcasted_iota(jnp.int32, (256, 256), 0)
    c = lax.broadcasted_iota(jnp.int32, (256, 256), 1)
    from_row = jnp.where((c >= 64) & (c < 128), c + 64, jnp.where((c >= 128) & (c < 192), c - 64, c))
    return jnp.where(r == from_row, 1.0, 0.0).astype(BF16)


def lifted(pairs):
    r = lax.broadcasted_iota(jnp.int32, (128, 256), 0)
    c = lax.broadcasted_iota(jnp.int32, (128, 256), 1)
    out = jnp.zeros((128, 256), F32)
    for row, col, scale in pairs:
        out = jnp.where((c >= col) & (c < col + 64) & (r - row == c - col), scale, out)
    return out.astype(BF16)


def layer_kernel(
    q_ref, k_ref, v_ref, gate_ref, info_ref, res_ref, mixg_ref, ffng_ref,
    wo_any, sg_any, su_any, sd_any, eg_any, eu_any, ed_any,
    o_ref,
    wo, sg, su, sd, eg, eu, ed, outgoing, arrived, result, received, acc, normed,
    qkv_out, qkv_in, q_all, k_all, v_all, scores, att_out, heads_in, heads, info, pack_code, pack_weight, ag_z, ag_x, ag_y,
    send_z, send_x, send_y, get_z, get_x, get_y,
    wsem, ready, out_s, out_r, ret_s, ret_r, qkv_s, qkv_r, att_s, att_r, info_s, info_r, ag_s, ag_r, part_s, part_r,
):
    loads = [
        pltpu.make_async_copy(src, dst, wsem.at[i])
        for i, (src, dst) in enumerate(
            [(wo_any, wo), (sg_any, sg), (su_any, su), (sd_any, sd), (eg_any, eg), (eu_any, eu), (ed_any, ed)]
        )
    ]
    me = lax.axis_index("sp")
    barrier = pltpu.get_barrier_semaphore()

    torus = Torus()
    dp = lax.axis_index("dp")
    row = [torus.sp[k % 4][(k // 4 + k) % 4] for k in range(1, 16)]
    column = [torus.dp[k // 2][k % 2] for k in range(1, 8)]
    for to in row:
        pl.semaphore_signal(barrier, inc=1, device_id=(to, dp), device_id_type=MESH)
    for to in column:
        pl.semaphore_signal(barrier, inc=1, device_id=(me, to), device_id_type=MESH)
    for c in loads:
        c.start()

    swap = swap_matrix()
    for p in range(8):
        cols = slice(p * 128, (p + 1) * 128)
        qk = dot(jnp.concatenate([q_ref[:, cols], k_ref[:, cols]], axis=1), swap).astype(BF16)
        vv = dot(jnp.concatenate([v_ref[:64, cols], v_ref[64:, cols]], axis=1), swap).astype(BF16)
        for side in range(2):
            part = slice(side * 128, (side + 1) * 128)
            qkv_out[2 * p + side, :128, :] = qk[:, part]
            qkv_out[2 * p + side, 128:, :] = vv[:, part]
    qkv_in[me] = qkv_out[me]

    pl.semaphore_wait(barrier, 22)

    for to in row:
        pltpu.make_async_remote_copy(
            src_ref=qkv_out.at[to], dst_ref=qkv_in.at[me], send_sem=qkv_s, recv_sem=qkv_r,
            device_id=(to, dp), device_id_type=MESH,
        ).start()

    def info_copy(axis, d):
        return pltpu.make_async_remote_copy(
            src_ref=info_ref, dst_ref=info.at[axis * 3 + d - 1], send_sem=info_s, recv_sem=info_r,
            device_id=torus.along(axis, d), device_id_type=MESH,
        )

    for axis in range(3):
        for d in range(1, 4):
            info_copy(axis, d).start()

    def expert_at(dz, dx, dy, dc):
        return (((torus.z + dz) & 3) * 4 + ((torus.x + dx) & 3)) * 8 + ((torus.y + dy) & 3) * 2 + ((torus.c + dc) & 1)

    earlier = jnp.where(
        lax.broadcasted_iota(jnp.int32, (PEERS, PEERS), 0) < lax.broadcasted_iota(jnp.int32, (PEERS, PEERS), 1),
        1.0,
        0.0,
    ).astype(BF16)

    def named_in(rows, peer):
        named = jnp.zeros((peer.shape[0], PEERS), F32)
        share = jnp.zeros((peer.shape[0], PEERS), F32)
        for j in range(4):
            hit = rows[j : j + 1, :] == peer
            named = jnp.where(hit, 1.0, named)
            share = jnp.where(hit, rows[4 + j : 5 + j, :], share)
        return named, share

    def ranked(named):
        return jnp.where(named > 0.5, dot(named.astype(BF16), earlier), -1.0)

    jth = lax.broadcasted_iota(jnp.int32, (PER, 1), 0)
    jc, ja, jb = jth >> 4, (jth >> 2) & 3, jth & 3
    js = (ja & 1) * 2 + (ja >> 1)
    planes = [expert_at(0, ja, jb, jc), expert_at(js, 0, jb, jc), expert_at(js, jb, 0, jc)]
    planes = [p.astype(F32) for p in planes]
    pltpu.make_async_copy(info, info, info_r).wait()
    for axis in range(3):
        parts = [named_in(info_ref[...], planes[axis])]
        for d in range(1, 4):
            parts.append(named_in(info[axis * 3 + d - 1], planes[axis]))
        pack_code[axis] = ranked(jnp.concatenate([p[0] for p in parts], axis=0))
        pack_weight[axis] = jnp.concatenate([p[1] for p in parts], axis=0)

    pltpu.make_async_copy(qkv_in.at[pl.ds(0, 15)], qkv_in.at[pl.ds(0, 15)], qkv_r).wait()

    split_qk = lifted([(0, 0, HEAD_DIM**-0.5), (64, 128, 1.0)])
    split_v = lifted([(0, 0, 1.0), (0, 64, 1.0), (64, 128, 1.0), (64, 192, 1.0)])
    for j in range(16):
        rows = slice(j * 128, (j + 1) * 128)
        qk = dot(qkv_in[j, :128, :], split_qk).astype(BF16)
        vv = dot(qkv_in[j, 128:, :], split_v).astype(BF16)
        q_all[rows, :] = qk[:, :128]
        k_all[rows, :] = qk[:, 128:]
        v_all[j * 128 : j * 128 + 64, :] = vv[:, :128]
        v_all[j * 128 + 64 : (j + 1) * 128, :] = vv[:, 128:]

    left = lax.broadcasted_iota(jnp.int32, (64, 128), 1) < 64
    ahead = lax.broadcasted_iota(jnp.int32, (256, 256), 1) - lax.broadcasted_iota(jnp.int32, (256, 256), 0)

    def att_copy(b):
        return pltpu.make_async_remote_copy(
            src_ref=att_out.at[b], dst_ref=heads_in.at[me], send_sem=att_s, recv_sem=att_r,
            device_id=(b, dp), device_id_type=MESH,
        )

    def attend(step, _):
        turn = (me // 2 + step) % 8
        q = q_all[pl.ds(pl.multiple_of(turn * 256, 256), 256), :]
        for group in range(4):

            @pl.when(turn // 2 == group)
            def _():
                last = group * 512
                parts = [slice(c, c + 256) for c in range(0, last + 512, 256)]
                base = gate_ref[:, last : last + 1]
                top = None
                for part in parts:
                    s = lax.dot_general(
                        q, k_all[part, :], (((1,), (1,)), ((), ())), preferred_element_type=F32
                    ) + (base - gate_ref[:, part])
                    if part.start >= last:
                        s = jnp.where(ahead <= (turn % 2) * 256 - (part.start - last), s, -jnp.inf)
                    scores[:, part] = s
                    peak = jnp.maximum(s[:, :128], s[:, 128:])
                    top = peak if top is None else jnp.maximum(top, peak)
                top = jnp.max(top, axis=1, keepdims=True)
                total = None
                for part in parts:
                    e = jnp.exp(scores[:, part] - top)
                    scores[:, part] = e
                    both = e[:, :128] + e[:, 128:]
                    total = both if total is None else total + both
                inverse = 1.0 / jnp.sum(total, axis=1, keepdims=True)
                o = None
                for part in parts:
                    piece = dot((scores[:, part] * inverse).astype(BF16), v_all[part, :])
                    o = piece if o is None else o + piece
                o = o.astype(BF16)
                att_out[2 * turn] = jnp.where(left, o[:64], o[64:128])
                att_out[2 * turn + 1] = jnp.where(left, o[128:192], o[192:])

        for half in range(2):
            b = 2 * turn + half

            @pl.when(b != me)
            def _():
                att_copy(b).start()

            @pl.when(b == me)
            def _():
                heads_in[me] = att_out[me]

        return 0

    lax.fori_loop(0, 8, attend, 0)
    pltpu.make_async_copy(heads_in.at[pl.ds(0, 15)], heads_in.at[pl.ds(0, 15)], att_r).wait()
    for to in column:
        pl.semaphore_signal(ready, inc=1, device_id=(me, to), device_id_type=MESH)
    for p in range(8):
        two = dot(jnp.concatenate([heads_in[2 * p], heads_in[2 * p + 1]], axis=1), swap).astype(BF16)
        heads[:64, p * 128 : (p + 1) * 128] = two[:, :128]
        heads[64:, p * 128 : (p + 1) * 128] = two[:, 128:]

    loads[0].wait()
    projected = dot(heads[...], wo[...])
    mixed = res_ref[...].astype(F32) + mixg_ref[...] * projected * lax.rsqrt(
        jnp.mean(projected * projected, axis=1, keepdims=True) + 1e-06
    )
    acc[...] = mixed
    normed[...] = (
        ffng_ref[...] * mixed * lax.rsqrt(jnp.mean(mixed * mixed, axis=1, keepdims=True) + 1e-06)
    ).astype(BF16)
    pl.semaphore_wait(ready, 7)

    def slots_of(ranks, values):
        r = lax.broadcasted_iota(jnp.int32, (PER, SLOTS, PEERS), 1).astype(F32)
        return jnp.where(ranks[:, None, :] == r, values, 0.0).reshape(PER * SLOTS, PEERS)

    gathered = (ag_z, ag_x, ag_y)
    for d in (2, 1, 3):
        for axis in range(3):
            pltpu.make_async_remote_copy(
                src_ref=normed.at[:, CUTS[axis]], dst_ref=gathered[axis].at[d - 1], send_sem=ag_s.at[axis], recv_sem=ag_r.at[axis],
                device_id=torus.along(axis, d), device_id_type=MESH,
            ).start()

    def pack(axis, d):
        cut = CUTS[axis]
        source = normed[:, cut] if d == 0 else gathered[axis][d - 1]
        place = slots_of(pack_code[axis, d * PER : (d + 1) * PER, :], 1.0).astype(BF16)
        rows = dot(place, source)
        box = lane_of(axis, d, slice(None), slice(None), slice(None))
        outgoing[(*box, slice(None), cut)] = rows.reshape(2, 4, 4, SLOTS, rows.shape[1]).astype(BF16)

    def send_planes(d, axes, cores):
        for dc in cores:
            for m in range(16):
                for axis in axes:
                    a, b = m % 4, (m // 4 + m) % 4
                    if axis == 1:
                        a, b = b, a
                    box = (*lane_of(axis, d, dc, a, b), slice(None), CUTS[axis])
                    if (dc, a, b) == (0, 0, 0):
                        arrived[box] = outgoing[box]
                        continue
                    way = [a, b]
                    way.insert(axis, 0)
                    pltpu.make_async_remote_copy(
                        src_ref=outgoing.at[box], dst_ref=arrived.at[box],
                        send_sem=out_s.at[dc], recv_sem=out_r.at[dc],
                        device_id=torus.at(*way, dc), device_id_type=MESH,
                    ).start()

    for axis in range(3):
        pack(axis, 0)
    send_planes(0, range(3), (0, 1))
    for axis in range(3):
        pltpu.make_async_copy(gathered[axis], gathered[axis], ag_r.at[axis]).wait()
        for d in range(1, 4):
            pack(axis, d)
    send_planes(slice(1, 4), range(3), (0, 1))

    def taken(ref, sem, *boxes):
        for box in boxes:
            part = ref.at[box]
            pltpu.make_async_copy(part, part, sem).wait()

    def wait_planes(ref, sem, dc):
        @pl.when(dc == 0)
        def _():
            taken(ref, sem.at[0], (0, *[slice(None)] * 4, slice(0, 1920)))

        @pl.when(dc == 1)
        def _():
            taken(ref, sem.at[1], (1,))

    def wait_back(ref, sem, dc, own):
        whole, most = slice(None), slice(0, 1920)
        if dc == 0:
            box = (0, 0, whole, whole, whole, most) if own else (0, pl.ds(0, 3), whole, whole, whole, most)
        else:
            box = (1, 3) if own else (1, pl.ds(0, 3))
        taken(ref, sem.at[dc * 2 + own], box)

    def send_back(dc):
        for own, d in enumerate([slice(1, 4), 0]):
            for m in range(16):
                for axis in range(3):
                    a, b = m % 4, (m // 4 + m) % 4
                    if axis == 1:
                        a, b = b, a
                    box = (*lane_of(axis, d, dc, a, b), slice(None), CUTS[axis])
                    way = [a, b]
                    way.insert(axis, 0)

                    def remote():
                        pltpu.make_async_remote_copy(
                            src_ref=result.at[box], dst_ref=received.at[box],
                            send_sem=ret_s.at[dc * 2 + own], recv_sem=ret_r.at[dc * 2 + own],
                            device_id=torus.back(*way, dc), device_id_type=MESH,
                        ).start()

                    if (a, b) == (0, 0):

                        @pl.when(dc == 0)
                        def _():
                            received[box] = result[box]

                        pl.when(dc > 0)(remote)
                    else:
                        remote()

    def combined(axis, d):
        box = lane_of(axis, d, slice(None), slice(None), slice(None))
        rows = received[(*box, slice(None), CUTS[axis])]
        rows = rows.astype(F32).reshape(PER * SLOTS, rows.shape[4]).astype(BF16)
        part = slice(d * PER, (d + 1) * PER)
        w = slots_of(pack_code[axis, part, :], pack_weight[axis, part, :][:, None, :])
        hi = w.astype(BF16)
        lo = (w - hi.astype(F32)).astype(BF16)
        dims = (((0,), (0,)), ((), ()))
        return lax.dot_general(hi, rows, dims, preferred_element_type=F32) + lax.dot_general(
            lo, rows, dims, preferred_element_type=F32
        )

    for c in loads[1:4]:
        c.wait()
    gate = dot(normed[...], sg[...])
    up = dot(normed[...], su[...])
    hidden = (gate / (1.0 + jnp.exp(-gate)) * up).astype(BF16)
    acc[...] += dot(hidden, sd[...])
    for c in loads[4:]:
        c.wait()

    def expert(dc, h):
        here = (dc, pl.ds(h * 2, 2))
        rows = arrived[here].astype(F32).reshape(PER * SLOTS, arrived.shape[5]).astype(BF16)
        g = dot(rows, eg[...])
        u = dot(rows, eu[...])
        hid = (g / (1.0 + jnp.exp(-g)) * u).astype(BF16)
        y = dot(hid, ed[...])
        result[here] = y.reshape(2, 4, 4, SLOTS, y.shape[1]).astype(BF16)
        return dc

    def experts(dc, _):
        wait_planes(arrived, out_r, dc)
        lax.fori_loop(0, 2, lambda h, core: expert(core, h), dc)
        send_back(dc)
        return 0

    lax.fori_loop(0, 2, experts, 0)

    sends, gets = (send_z, send_x, send_y), (get_z, get_x, get_y)
    wait_back(received, ret_r, 0, 0)
    wait_back(received, ret_r, 0, 1)
    wait_back(received, ret_r, 1, 0)
    for d in (2, 1, 3):
        for axis in range(3):
            sends[axis][d - 1] = combined(axis, d).astype(BF16)
            pltpu.make_async_remote_copy(
                src_ref=sends[axis].at[d - 1], dst_ref=gets[axis].at[d - 1],
                send_sem=part_s.at[axis], recv_sem=part_r.at[axis],
                device_id=torus.along(axis, -d), device_id_type=MESH,
            ).start()
    wait_back(received, ret_r, 1, 1)
    for axis in range(3):
        acc[:, CUTS[axis]] += combined(axis, 0)
    for axis in range(3):
        pltpu.make_async_copy(gets[axis], gets[axis], part_r.at[axis]).wait()
        add = gets[axis][0].astype(F32) + gets[axis][1].astype(F32) + gets[axis][2].astype(F32)
        acc[:, CUTS[axis]] += add
    o_ref[...] = acc[...].astype(BF16)

    pltpu.make_async_copy(qkv_out.at[pl.ds(0, 15)], qkv_out.at[pl.ds(0, 15)], qkv_s).wait()
    pltpu.make_async_copy(att_out.at[pl.ds(0, 15)], att_out.at[pl.ds(0, 15)], att_s).wait()

    pltpu.make_async_copy(info, info, info_s).wait()
    for axis in range(3):
        pltpu.make_async_copy(gathered[axis], gathered[axis], ag_s.at[axis]).wait()
    for dc in range(2):
        wait_planes(outgoing, out_s, dc)

    for dc in range(2):
        for own in range(2):
            wait_back(result, ret_s, dc, own)
    for axis in range(3):
        pltpu.make_async_copy(sends[axis], sends[axis], part_s.at[axis]).wait()


def layer(q, k, v, gates, info, residual, mix_gain, ffn_gain, *weights):
    tok, width = residual.shape
    length = gates.shape[1]
    vm, hbm = pl.BlockSpec(memory_space=pltpu.VMEM), pl.BlockSpec(memory_space=pl.ANY)
    boxes = pltpu.VMEM((2, 4, 4, 4, SLOTS, width), BF16)
    dma, dma_groups = pltpu.SemaphoreType.DMA, pltpu.SemaphoreType.DMA((GROUPS,))
    return pl.pallas_call(
        layer_kernel,
        out_shape=jax.ShapeDtypeStruct((tok, width), BF16),
        in_specs=[vm] * 8 + [hbm] * 7,
        out_specs=vm,
        scratch_shapes=[pltpu.VMEM(w.shape, w.dtype) for w in weights]
        + [boxes] * 4
        + [pltpu.VMEM((tok, width), F32), pltpu.VMEM((tok, width), BF16)]
        + [pltpu.VMEM((16, 192, 128), BF16)] * 2
        + [pltpu.VMEM((length, 128), BF16)] * 3
        + [pltpu.VMEM((256, length), F32)]
        + [pltpu.VMEM((16, 64, 128), BF16)] * 2
        + [pltpu.VMEM((tok, 1024), BF16)]
        + [pltpu.VMEM((9, 8, tok), F32)]
        + [pltpu.VMEM((3, PEERS, PEERS), F32)] * 2
        + [pltpu.VMEM((3, tok, cut.stop - cut.start), BF16) for cut in CUTS] * 3
        + [dma((7,)), pltpu.SemaphoreType.REGULAR]
        + [pltpu.SemaphoreType.DMA((2,))] * 2
        + [dma_groups] * 2
        + [dma] * 6
        + [dma((3,))] * 4,
        compiler_params=pltpu.CompilerParams(
            collective_id=1, has_side_effects=True, vmem_limit_bytes=60 * 2**20
        ),
        name="layer",
    )(q, k, v, gates, info, residual, mix_gain[None], ffn_gain[None], *weights)


def shards(
    residual_in,
    query_rows,
    key_rows,
    value_rows,
    gate_sums,
    out_weight,
    mix_gain,
    ffn_gain,
    expert_ids,
    route_weights,
    expert_gate,
    expert_up,
    expert_down,
    shared_gate,
    shared_up,
    shared_down,
):
    info = jnp.concatenate([expert_ids[0].astype(F32), route_weights[0]], axis=1).T
    return layer(
        query_rows[0], key_rows[0], value_rows[0], gate_sums[0], info,
        residual_in[0], mix_gain, ffn_gain, out_weight,
        shared_gate, shared_up, shared_down, expert_gate[0], expert_up[0], expert_down[0],
    )[None]


def solution(mesh):
    return jax.shard_map(
        shards,
        mesh=mesh,
        in_specs=(
            P("dp", "sp", None),
            P("dp", "sp", None),
            P("dp", "sp", None),
            P("dp", "sp", None),
            P("dp", "sp", None),
            P(),
            P(),
            P(),
            P("dp", "sp", None),
            P("dp", "sp", None),
            P(("sp", "dp"), None, None),
            P(("sp", "dp"), None, None),
            P(("sp", "dp"), None, None),
            P(),
            P(),
            P(),
        ),
        out_specs=P("dp", "sp", None),
        check_vma=False,
    )
```
